32 devices in a mesh: sp: 16 (over z, y, x), tp: 2 (over core).
Axes of the slice: x: 2, y: 2, z: 4, core: 2. Of those that a mesh axis runs over, the one named last changes fastest.
Arguments:
- queries: bfloat16 [6144, 2048], P('sp', 'tp'), may hold values from -6 to 6
- key_heads: bfloat16 [6144, 1024], P('sp', 'tp'), may hold values from -6 to 6
- value_heads: bfloat16 [6144, 1024], P('sp', 'tp'), may hold values from -6 to 6
- sink_logit: float32 [16], P('tp'), may hold values from 3 to 7
- doc_ids: int32 [6144], replicated, may hold values from 0 to 3, never falling along the last dimension, each value on 1 to 3072 neighbouring positions
- residual: bfloat16 [6144, 2048], P('sp'), may hold values from -6 to 6
- out_proj: bfloat16 [2048, 2048], P('tp'), may hold values from -0.125 to 0.125
- gain_mix: float32 [2048], replicated, may hold values from 0.1 to 1.9
- up_proj: bfloat16 [2048, 8192], P('sp', 'tp'), may hold values from -0.125 to 0.125
- down_proj: bfloat16 [8192, 2048], P('tp', 'sp'), may hold values from -0.0625 to 0.0625
- gain_ffn_in: float32 [2048], replicated, may hold values from 0.1 to 1.9
- gain_ffn_out: float32 [2048], replicated, may hold values from 0.1 to 1.9
Outputs:
- layer_out: bfloat16 [6144, 2048], P(('sp', 'tp'))
The draws below stay inside these ranges and needn't reach their ends.
All inputs are finite; a program needn't handle non-finite values.
Results may differ from the reference program's by a relative error of at most 0.019.
Values may be sent and summed in bfloat16 or wider, within the bound.
A program may use at most 128 MiB of HBM per device.

```python
import math
import jax
import jax.numpy as jnp
import numpy as np
from jax import lax

D = 2048
HEADS = 16
KV = 8
HD = 128
FF = 8192
WINDOW = 128
TOKENS = 6144
DOCS = 4
DOC_MOST = 3072
N_TP = 2


def draw_key_heads(key, part):
    noise_key = jax.random.fold_in(key, 2)
    noise = jax.random.normal(noise_key, (TOKENS, KV * HD), jnp.float32)
    return jnp.clip(noise, -6.0, 6.0).astype(jnp.bfloat16)


def draw_queries(key, part):
    noise_key = jax.random.fold_in(key, 1)
    noise = jax.random.normal(noise_key, (TOKENS, HEADS * HD), jnp.float32)
    return jnp.clip(noise, -6.0, 6.0).astype(jnp.bfloat16)


def level_of(key, extent, pieces, low, largest):
    loudness, own = 1.0, jax.random.fold_in(key, 6)
    for axis_at, shards_of in pieces:
        heights = jnp.exp(jax.random.uniform(jax.random.fold_in(own, axis_at), (shards_of,), jnp.float32, low / len(pieces), largest / len(pieces)))
        loudness = loudness * jnp.repeat(heights, extent[axis_at] // shards_of).reshape([-1 if axis == axis_at else 1 for axis in range(len(extent))])
    return loudness


def length_profile(amount, total, bound, slope):
    loads = [(1 << 20) // math.isqrt(rank ** slope) + 1 for rank in range(2, amount + 1)]
    spare, holding = total - bound - (amount - 1), [1] * (amount - 1)
    while spare > 0:
        movable = [i for i in range(amount - 1) if holding[i] < bound]
        mass, budget = sum([loads[i] for i in movable]), spare
        for i in movable:
            extra = min(bound - holding[i], max(1, budget * loads[i] // mass), spare)
            holding[i] = holding[i] + extra
            spare = spare - extra
    return np.array([bound] + holding)


def uneven_parts(own_key, amount, total, most, skew):
    if amount == 2:
        one = jax.random.randint(own_key, (), max(1, total - most), min(most, total - 1) + 1)
        return jnp.stack([one, total - one])
    sizes = jnp.asarray(length_profile(amount, total, most, skew), jnp.int32)
    couples = (amount - 1) // 2
    donor, sink = sizes[1:1 + 2 * couples:2], sizes[2:2 + 2 * couples:2]
    room = jnp.minimum(donor - 1, most - sink)
    shifted = jax.random.randint(jax.random.fold_in(own_key, 1), (couples,), 0, 1 << 20) % (room + 1)
    sizes = sizes.at[1:1 + 2 * couples:2].set(donor - shifted).at[2:2 + 2 * couples:2].set(sink + shifted)
    return sizes[jax.random.permutation(jax.random.fold_in(own_key, 2), amount)]


def centred(rng, dims, spread, bound, cuts=(), held_as=jnp.bfloat16):
    array = spread * jax.random.normal(rng, dims, jnp.float32)
    if cuts:
        array = array * level_of(rng, dims, cuts, -0.22, 0.18)
    return jnp.clip(array, -bound, bound).astype(held_as)


def setup_inputs(seed: int = 0) -> dict:
    keys = jax.random.split(jax.random.key(seed), 13)
    return {
        "queries": draw_queries(jax.random.fold_in(keys[12], 71), 0),
        "key_heads": draw_key_heads(jax.random.fold_in(keys[12], 71), 0),
        "value_heads": centred(keys[2], (TOKENS, KV * HD), 1.0, 6.0, ((0, 16), (1, 2))),
        "sink_logit": jnp.clip(3.0 + 4.0 * jax.random.uniform(keys[3], (HEADS,), jnp.float32) ** level_of(keys[3], (HEADS,), ((0, 2),), -0.2, 0.2), 3.0, 7.0),
        "doc_ids": jnp.searchsorted(jnp.cumsum(uneven_parts(keys[4], DOCS, TOKENS, DOC_MOST, 1)), jnp.arange(TOKENS), side="right").astype(jnp.int32),
        "residual": centred(keys[5], (TOKENS, D), 1.0, 6.0, ((0, 16),)),
        "out_proj": centred(keys[6], (HEADS * HD, D), (HEADS * HD) ** -0.5, 0.125, ((0, 2),)),
        "gain_mix": jnp.clip(1.0 + 0.18 * jax.random.normal(keys[7], (D,), jnp.float32), 0.1, 1.9),
        "up_proj": centred(keys[8], (D, FF), D ** -0.5, 0.125, ((0, 16), (1, 2))),
        "down_proj": centred(keys[9], (FF, D), FF ** -0.5, 0.0625, ((0, 2), (1, 16))),
        "gain_ffn_in": jnp.clip(1.0 + 0.18 * jax.random.normal(keys[10], (D,), jnp.float32), 0.1, 1.9),
        "gain_ffn_out": jnp.clip(1.0 + 0.18 * jax.random.normal(keys[11], (D,), jnp.float32), 0.1, 1.9),
    }


def rotate(field, places):
    half_dim = HD // 2
    inv_freq = 10000.0 ** (-jnp.arange(0, HD, 2, dtype=jnp.float32) / HD)
    angles = places[:, None, None] * inv_freq[None, None, :]
    cosine = jnp.cos(angles)
    sine = jnp.sin(angles)
    lower = field[..., :half_dim].astype(jnp.float32)
    upper = field[..., half_dim:].astype(jnp.float32)
    return jnp.concatenate([lower * cosine - upper * sine, upper * cosine + lower * sine], axis=-1).astype(jnp.bfloat16)

def banded(field, blocks):
    framed = field.reshape((blocks + 2, WINDOW) + field.shape[1:])
    return jnp.concatenate([framed[:-2], framed[1:-1], framed[2:]], axis=1)

def rms_scale(field, gain_vec):
    return field * lax.rsqrt(lax.optimization_barrier(jnp.mean(field * field, axis=-1, keepdims=True)) + 1e-06) * gain_vec

def reference(queries, key_heads, value_heads, sink_logit, doc_ids, residual, out_proj, gain_mix, up_proj, down_proj, gain_ffn_in, gain_ffn_out):
    length = queries.shape[0]
    blocks = length // WINDOW
    group_size = HEADS // KV
    places = jnp.arange(length).astype(jnp.float32)
    rotated_q = rotate(queries.reshape(length, HEADS, HD), places).reshape(blocks, WINDOW, KV, group_size, HD)
    rotated_k = rotate(key_heads.reshape(length, KV, HD), places)
    framing = ((WINDOW, WINDOW), (0, 0), (0, 0))
    key_win = banded(jnp.pad(rotated_k, framing), blocks)
    val_win = banded(jnp.pad(value_heads.reshape(length, KV, HD), framing), blocks)
    key_docs = banded(jnp.pad(doc_ids, (WINDOW, WINDOW), constant_values=-1), blocks)
    query_docs = doc_ids.reshape(blocks, WINDOW)
    q_index = jnp.arange(WINDOW)[:, None]
    k_index = jnp.arange(3 * WINDOW)[None, :]
    in_window = jnp.abs(k_index - WINDOW - q_index) <= WINDOW
    allowed = in_window[None] & (query_docs[:, :, None] == key_docs[:, None, :])

    def one_head(items):
        q_head, k_head, v_head, sink_vec = items
        scores = jnp.einsum('nqgd,nsd->ngqs', q_head.astype(jnp.float32), k_head.astype(jnp.float32)) * HD ** (-0.5)
        masked = jnp.where(allowed[:, None], scores, -1e+30)
        sink_col = sink_vec[None, :, None]
        top_score = jnp.maximum(lax.optimization_barrier(jnp.max(masked, axis=-1)), sink_col)
        exp_scores = jnp.where(allowed[:, None], jnp.exp(masked - top_score[..., None]), 0.0)
        denom_sum = lax.optimization_barrier(jnp.sum(exp_scores, axis=-1)) + jnp.exp(sink_col - top_score)
        probs = (exp_scores / denom_sum[..., None]).astype(jnp.bfloat16)
        return jnp.einsum('ngqs,nsd->nqgd', probs.astype(jnp.float32), v_head.astype(jnp.float32)).astype(jnp.bfloat16)
    attended = lax.map(one_head, (jnp.moveaxis(rotated_q, 2, 0), jnp.moveaxis(key_win, 2, 0), jnp.moveaxis(val_win, 2, 0), sink_logit.reshape(KV, group_size)))
    attn = jnp.moveaxis(attended, 0, 2).reshape(length, HEADS * HD)
    attn_cols = HEADS * HD // N_TP
    mixed = jnp.zeros((length, D), jnp.float32)
    for group in range(N_TP):
        partial_value = jnp.dot(attn[:, group * attn_cols:(group + 1) * attn_cols], out_proj[group * attn_cols:(group + 1) * attn_cols], preferred_element_type=jnp.float32).astype(jnp.bfloat16)
        mixed = mixed + lax.optimization_barrier(partial_value).astype(jnp.float32)
    after_mix = (residual.astype(jnp.float32) + rms_scale(mixed, gain_mix)).astype(jnp.bfloat16)
    normed = rms_scale(after_mix.astype(jnp.float32), gain_ffn_in).astype(jnp.bfloat16)
    hid_cols = FF // N_TP
    ffn_out = jnp.zeros((length, D), jnp.float32)
    for group in range(N_TP):
        up_acts = jnp.dot(normed, up_proj[:, group * hid_cols:(group + 1) * hid_cols], preferred_element_type=jnp.float32)
        hidden = jnp.square(jax.nn.relu(up_acts)).astype(jnp.bfloat16)
        partial_value = jnp.dot(hidden, down_proj[group * hid_cols:(group + 1) * hid_cols], preferred_element_type=jnp.float32).astype(jnp.bfloat16)
        ffn_out = ffn_out + lax.optimization_barrier(partial_value).astype(jnp.float32)
    return (after_mix.astype(jnp.float32) + rms_scale(ffn_out, gain_ffn_out)).astype(jnp.bfloat16)
```

```python
import math

import jax
import jax.numpy as jnp
from jax import lax
from jax.sharding import Mesh, PartitionSpec as P

HD = 128
WINDOW = 128
SP = ("a", "b", "c", "d")
GRP = ("c", "d")
CROSS = ("a", "b")


def padded(shard, sides, width):
    for axis, dim in sides:
        devices, length = (lax.axis_size(axis), shard.shape[dim])
        up = [(i, (i + 1) % devices) for i in range(devices - 1)]
        down = [(j, i) for i, j in up]
        last = lax.slice_in_dim(shard, length - width, length, axis=dim)
        first = lax.slice_in_dim(shard, 0, width, axis=dim)
        before = lax.ppermute(last, axis, up)
        after = lax.ppermute(first, axis, down)
        shard = jnp.concatenate([before, shard, after], axis=dim)
    return shard


def rotate(field, places):
    half_dim = HD // 2
    inv_freq = 10000.0 ** (-jnp.arange(0, HD, 2, dtype=jnp.float32) / HD)
    angles = places[:, None, None] * inv_freq[None, None, :]
    cosine = jnp.cos(angles)
    sine = jnp.sin(angles)
    lower = field[..., :half_dim].astype(jnp.float32)
    upper = field[..., half_dim:].astype(jnp.float32)
    return jnp.concatenate(
        [lower * cosine - upper * sine, upper * cosine + lower * sine], axis=-1
    ).astype(jnp.bfloat16)


def banded(field, blocks):
    framed = field.reshape((blocks + 2, WINDOW) + field.shape[1:])
    return jnp.concatenate([framed[:-2], framed[1:-1], framed[2:]], axis=1)


def rms_scale(field, gain_vec):
    return field * lax.rsqrt(jnp.mean(field * field, axis=-1, keepdims=True) + 1e-06) * gain_vec


def swap_tp(rows):
    return lax.ppermute(rows, "tp", [(0, 1), (1, 0)])


def gather_tp(rows):
    if lax.axis_size("tp") == 2:
        return jnp.concatenate([rows, swap_tp(rows)], axis=0)
    return lax.all_gather(rows, "tp", axis=0, tiled=True)


def scatter_tp(partial_value, own_first=True):
    devices = lax.axis_size("tp")
    if devices != 2:
        return lax.psum_scatter(partial_value, "tp", scatter_dimension=0, tiled=True).astype(
            jnp.float32
        )
    share = partial_value.shape[0] // 2
    if own_first:
        own, other = partial_value[:share], partial_value[share:]
    else:
        me = lax.axis_index("tp")
        own = lax.dynamic_slice_in_dim(partial_value, me * share, share, 0)
        other = lax.dynamic_slice_in_dim(partial_value, (1 - me) * share, share, 0)
    return own.astype(jnp.float32) + swap_tp(other).astype(jnp.float32)


def to_peer(rows, k):
    if k == 0:
        return rows
    return lax.ppermute(rows, GRP, [(i, i ^ k) for i in range(4)])


def body(
    queries,
    key_heads,
    value_heads,
    sink_logit,
    doc_ids,
    residual,
    out_proj,
    gain_mix,
    up_proj,
    down_proj,
    gain_ffn_in,
    gain_ffn_out,
):
    up_quarter = lax.all_to_all(up_proj, GRP, split_axis=1, concat_axis=0, tiled=True)
    down_quarter = lax.all_to_all(down_proj, GRP, split_axis=0, concat_axis=1, tiled=True)
    queries, key_heads, up_quarter, down_quarter = lax.optimization_barrier(
        (queries, key_heads, up_quarter, down_quarter)
    )
    half_units = up_quarter.shape[1] // 2
    up_early = lax.all_gather(up_quarter[:, :half_units], CROSS, axis=0, tiled=True)
    up_late = lax.all_gather(up_quarter[:, half_units:], CROSS, axis=0, tiled=True)
    down_all = lax.all_gather(down_quarter, CROSS, axis=0, tiled=False)
    tok_count = queries.shape[0]
    blocks = tok_count // WINDOW
    share_rows = tok_count // lax.axis_size("tp")
    q_local = queries.shape[1] // HD
    kv_local = key_heads.shape[1] // HD
    group_size = q_local // kv_local
    offset = lax.axis_index(SP) * tok_count
    places = (offset + jnp.arange(tok_count)).astype(jnp.float32)
    rotated_q = rotate(queries.reshape(tok_count, q_local, HD), places).reshape(
        blocks, WINDOW, kv_local, group_size, HD
    )
    rotated_k = rotate(key_heads.reshape(tok_count, kv_local, HD), places).reshape(
        tok_count, kv_local * HD
    )
    rimmed = padded(jnp.stack([rotated_k, value_heads]), ((SP, 1),), WINDOW)
    key_win = banded(rimmed[0].reshape(-1, kv_local, HD), blocks)
    val_win = banded(rimmed[1].reshape(-1, kv_local, HD), blocks)
    padded_docs = jnp.pad(doc_ids, (WINDOW, WINDOW), constant_values=-1)
    key_docs = banded(lax.dynamic_slice_in_dim(padded_docs, offset, tok_count + 2 * WINDOW), blocks)
    query_docs = lax.dynamic_slice_in_dim(doc_ids, offset, tok_count).reshape(blocks, WINDOW)
    q_index = jnp.arange(WINDOW)[:, None]
    k_index = jnp.arange(3 * WINDOW)[None, :]
    in_window = jnp.abs(k_index - WINDOW - q_index) <= WINDOW
    allowed = (in_window[None] & (query_docs[:, :, None] == key_docs[:, None, :]))[:, None, None]
    scores = jnp.einsum(
        "nqkgd,nskd->nkgqs", rotated_q, key_win, preferred_element_type=jnp.float32
    ) * HD ** (-0.5)
    masked = jnp.where(allowed, scores, -1e30)
    sink_col = sink_logit.reshape(kv_local, group_size)[None, :, :, None]
    top_score = jnp.maximum(jnp.max(masked, axis=-1), sink_col)
    exp_scores = jnp.where(allowed, jnp.exp(masked - top_score[..., None]), 0.0)
    denom_sum = jnp.sum(exp_scores, axis=-1) + jnp.exp(sink_col - top_score)
    probs = (exp_scores / denom_sum[..., None]).astype(jnp.bfloat16)
    attn = (
        jnp.einsum("nkgqs,nskd->nqkgd", probs, val_win, preferred_element_type=jnp.float32)
        .astype(jnp.bfloat16)
        .reshape(tok_count, q_local * HD)
    )
    part = jnp.dot(attn, out_proj, preferred_element_type=jnp.float32).astype(jnp.bfloat16)
    part, up_early = lax.optimization_barrier((part, up_early))
    mixed = scatter_tp(part, own_first=False)
    own_residual = lax.dynamic_slice_in_dim(
        residual, lax.axis_index("tp") * share_rows, share_rows, 0
    )
    after_mix = (own_residual.astype(jnp.float32) + rms_scale(mixed, gain_mix)).astype(jnp.bfloat16)
    normed = rms_scale(after_mix.astype(jnp.float32), gain_ffn_in).astype(jnp.bfloat16)
    sizes = [lax.axis_size(a) for a in SP]
    order = [SP.index(a) for a in CROSS + GRP]
    width = normed.shape[1]
    strip = width // math.prod(sizes)
    normed = (
        normed.reshape(share_rows, *sizes, strip)
        .transpose(0, *[1 + o for o in order], 5)
        .reshape(share_rows, width)
    )
    blocks = [to_peer(normed, k) for k in range(4)]
    partials = []
    for k in (3, 2, 1, 0):
        rows = gather_tp(blocks[k])
        hidden = jnp.concatenate(
            [
                jnp.square(
                    jax.nn.relu(jnp.dot(rows, w, preferred_element_type=jnp.float32))
                ).astype(jnp.bfloat16)
                for w in (up_early, up_late)
            ],
            axis=1,
        )
        partial_value = jnp.concatenate(
            [
                jnp.dot(hidden, down_all[i], preferred_element_type=jnp.float32).astype(jnp.bfloat16)
                for i in range(down_all.shape[0])
            ],
            axis=1,
        )
        partials.append(to_peer(scatter_tp(partial_value).astype(jnp.bfloat16), k))
    ffn_out = sum(p.astype(jnp.float32) for p in partials)
    back = [order.index(i) for i in range(4)]
    ffn_out = (
        ffn_out.reshape(share_rows, *[sizes[o] for o in order], strip)
        .transpose(0, *[1 + b for b in back], 5)
        .reshape(share_rows, width)
    )
    return (after_mix.astype(jnp.float32) + rms_scale(ffn_out, gain_ffn_out)).astype(jnp.bfloat16)


def solution(mesh):
    sp, tp = mesh.shape["sp"], mesh.shape["tp"]
    fine = Mesh(mesh.devices.reshape(sp // 8, 2, 2, 2, tp), SP + ("tp",))
    return jax.shard_map(
        body,
        mesh=fine,
        in_specs=(
            P(SP, "tp"),
            P(SP, "tp"),
            P(SP, "tp"),
            P("tp"),
            P(),
            P(SP, None),
            P("tp", None),
            P(),
            P(SP, "tp"),
            P("tp", SP),
            P(),
            P(),
        ),
        out_specs=P(SP + ("tp",), None),
        check_vma=False,
    )
```

```python
import math

import jax
import jax.numpy as jnp
from jax import lax
from jax.sharding import Mesh, PartitionSpec as P

HD = 128
WINDOW = 128
SP = ("a", "b", "c", "d")
GRP = ("c", "d")
CROSS = ("a", "b")


def padded(shard, sides, width):
    for axis, dim in sides:
        devices, length = (lax.axis_size(axis), shard.shape[dim])
        up = [(i, (i + 1) % devices) for i in range(devices - 1)]
        down = [(j, i) for i, j in up]
        last = lax.slice_in_dim(shard, length - width, length, axis=dim)
        first = lax.slice_in_dim(shard, 0, width, axis=dim)
        before = lax.ppermute(last, axis, up)
        after = lax.ppermute(first, axis, down)
        shard = jnp.concatenate([before, shard, after], axis=dim)
    return shard


def rotate(field, places):
    half_dim = HD // 2
    inv_freq = 10000.0 ** (-jnp.arange(0, HD, 2, dtype=jnp.float32) / HD)
    angles = places[:, None, None] * inv_freq[None, None, :]
    cosine = jnp.cos(angles)
    sine = jnp.sin(angles)
    lower = field[..., :half_dim].astype(jnp.float32)
    upper = field[..., half_dim:].astype(jnp.float32)
    return jnp.concatenate(
        [lower * cosine - upper * sine, upper * cosine + lower * sine], axis=-1
    ).astype(jnp.bfloat16)


def banded(field, blocks):
    framed = field.reshape((blocks + 2, WINDOW) + field.shape[1:])
    return jnp.concatenate([framed[:-2], framed[1:-1], framed[2:]], axis=1)


def rms_scale(field, gain_vec):
    return field * lax.rsqrt(jnp.mean(field * field, axis=-1, keepdims=True) + 1e-06) * gain_vec


def swap_tp(rows):
    return lax.ppermute(rows, "tp", [(0, 1), (1, 0)])


def gather_tp(rows):
    if lax.axis_size("tp") == 2:
        return jnp.concatenate([rows, swap_tp(rows)], axis=0)
    return lax.all_gather(rows, "tp", axis=0, tiled=True)


def scatter_tp(partial_value, own_first=True):
    devices = lax.axis_size("tp")
    if devices != 2:
        return lax.psum_scatter(partial_value, "tp", scatter_dimension=0, tiled=True).astype(
            jnp.float32
        )
    share = partial_value.shape[0] // 2
    if own_first:
        own, other = partial_value[:share], partial_value[share:]
    else:
        me = lax.axis_index("tp")
        own = lax.dynamic_slice_in_dim(partial_value, me * share, share, 0)
        other = lax.dynamic_slice_in_dim(partial_value, (1 - me) * share, share, 0)
    return own.astype(jnp.float32) + swap_tp(other).astype(jnp.float32)


def to_peer(rows, k):
    if k == 0:
        return rows
    return lax.ppermute(rows, GRP, [(i, i ^ k) for i in range(4)])


def line_gather(block, axis):
    n = lax.axis_size(axis)
    up = [(i, i + 1) for i in range(n - 1)]
    down = [(j, i) for i, j in up]
    held = [block]
    low, high = block, block
    for _ in range(n - 1):
        low, high = lax.ppermute(low, axis, up), lax.ppermute(high, axis, down)
        held = [low] + held + [high]
    return lax.dynamic_slice_in_dim(jnp.stack(held), n - 1 - lax.axis_index(axis), n, 0)


def body(
    queries,
    key_heads,
    value_heads,
    sink_logit,
    doc_ids,
    residual,
    out_proj,
    gain_mix,
    up_proj,
    down_proj,
    gain_ffn_in,
    gain_ffn_out,
):
    up_quarter = lax.all_to_all(up_proj, GRP, split_axis=1, concat_axis=0, tiled=True)
    down_quarter = lax.all_to_all(down_proj, GRP, split_axis=0, concat_axis=1, tiled=True)
    queries, key_heads, up_quarter, down_quarter = lax.optimization_barrier(
        (queries, key_heads, up_quarter, down_quarter)
    )
    half_units = up_quarter.shape[1] // 2
    up_early = lax.all_gather(up_quarter[:, :half_units], CROSS, axis=0, tiled=True)
    up_late = lax.all_gather(up_quarter[:, half_units:], CROSS, axis=0, tiled=True)
    down_all = line_gather(down_quarter, CROSS)
    tok_count = queries.shape[0]
    blocks = tok_count // WINDOW
    share_rows = tok_count // lax.axis_size("tp")
    q_local = queries.shape[1] // HD
    kv_local = key_heads.shape[1] // HD
    group_size = q_local // kv_local
    offset = lax.axis_index(SP) * tok_count
    places = (offset + jnp.arange(tok_count)).astype(jnp.float32)
    rotated_q = rotate(queries.reshape(tok_count, q_local, HD), places).reshape(
        blocks, WINDOW, kv_local, group_size, HD
    )
    rotated_k = rotate(key_heads.reshape(tok_count, kv_local, HD), places).reshape(
        tok_count, kv_local * HD
    )
    rimmed = padded(jnp.stack([rotated_k, value_heads]), ((SP, 1),), WINDOW)
    key_win = banded(rimmed[0].reshape(-1, kv_local, HD), blocks)
    val_win = banded(rimmed[1].reshape(-1, kv_local, HD), blocks)
    padded_docs = jnp.pad(doc_ids, (WINDOW, WINDOW), constant_values=-1)
    key_docs = banded(lax.dynamic_slice_in_dim(padded_docs, offset, tok_count + 2 * WINDOW), blocks)
    query_docs = lax.dynamic_slice_in_dim(doc_ids, offset, tok_count).reshape(blocks, WINDOW)
    q_index = jnp.arange(WINDOW)[:, None]
    k_index = jnp.arange(3 * WINDOW)[None, :]
    in_window = jnp.abs(k_index - WINDOW - q_index) <= WINDOW
    allowed = (in_window[None] & (query_docs[:, :, None] == key_docs[:, None, :]))[:, None, None]
    scores = jnp.einsum(
        "nqkgd,nskd->nkgqs", rotated_q, key_win, preferred_element_type=jnp.float32
    ) * HD ** (-0.5)
    masked = jnp.where(allowed, scores, -1e30)
    sink_col = sink_logit.reshape(kv_local, group_size)[None, :, :, None]
    top_score = jnp.maximum(jnp.max(masked, axis=-1), sink_col)
    exp_scores = jnp.where(allowed, jnp.exp(masked - top_score[..., None]), 0.0)
    denom_sum = jnp.sum(exp_scores, axis=-1) + jnp.exp(sink_col - top_score)
    probs = (exp_scores / denom_sum[..., None]).astype(jnp.bfloat16)
    attn = (
        jnp.einsum("nkgqs,nskd->nqkgd", probs, val_win, preferred_element_type=jnp.float32)
        .astype(jnp.bfloat16)
        .reshape(tok_count, q_local * HD)
    )
    part = jnp.dot(attn, out_proj, preferred_element_type=jnp.float32).astype(jnp.bfloat16)
    part, up_early = lax.optimization_barrier((part, up_early))
    mixed = scatter_tp(part, own_first=False)
    own_residual = lax.dynamic_slice_in_dim(
        residual, lax.axis_index("tp") * share_rows, share_rows, 0
    )
    after_mix = (own_residual.astype(jnp.float32) + rms_scale(mixed, gain_mix)).astype(jnp.bfloat16)
    normed = rms_scale(after_mix.astype(jnp.float32), gain_ffn_in).astype(jnp.bfloat16)
    sizes = [lax.axis_size(a) for a in SP]
    order = [SP.index(a) for a in CROSS + GRP]
    width = normed.shape[1]
    strip = width // math.prod(sizes)
    normed = (
        normed.reshape(share_rows, *sizes, strip)
        .transpose(0, *[1 + o for o in order], 5)
        .reshape(share_rows, width)
    )
    blocks = [to_peer(normed, k) for k in range(4)]
    partials = []
    for k in (3, 2, 1, 0):
        rows = gather_tp(blocks[k])
        hidden = jnp.concatenate(
            [
                jnp.square(
                    jax.nn.relu(jnp.dot(rows, w, preferred_element_type=jnp.float32))
                ).astype(jnp.bfloat16)
                for w in (up_early, up_late)
            ],
            axis=1,
        )
        partial_value = jnp.concatenate(
            [
                jnp.dot(hidden, down_all[i], preferred_element_type=jnp.float32).astype(jnp.bfloat16)
                for i in range(down_all.shape[0])
            ],
            axis=1,
        )
        partials.append(to_peer(scatter_tp(partial_value).astype(jnp.bfloat16), k))
    ffn_out = sum(p.astype(jnp.float32) for p in partials)
    back = [order.index(i) for i in range(4)]
    ffn_out = (
        ffn_out.reshape(share_rows, *[sizes[o] for o in order], strip)
        .transpose(0, *[1 + b for b in back], 5)
        .reshape(share_rows, width)
    )
    return (after_mix.astype(jnp.float32) + rms_scale(ffn_out, gain_ffn_out)).astype(jnp.bfloat16)


def solution(mesh):
    sp, tp = mesh.shape["sp"], mesh.shape["tp"]
    fine = Mesh(mesh.devices.reshape(sp // 8, 2, 2, 2, tp), SP + ("tp",))
    return jax.shard_map(
        body,
        mesh=fine,
        in_specs=(
            P(SP, "tp"),
            P(SP, "tp"),
            P(SP, "tp"),
            P("tp"),
            P(),
            P(SP, None),
            P("tp", None),
            P(),
            P(SP, "tp"),
            P("tp", SP),
            P(),
            P(),
        ),
        out_specs=P(SP + ("tp",), None),
        check_vma=False,
    )
```
